32 devices in a mesh: sp: 8 (over z, core), tp: 4 (over y, x).
Axes of the slice: x: 2, y: 2, z: 4, core: 2. Of those that a mesh axis runs over, the one named last changes fastest.
Arguments:
- residual: bfloat16 [1536, 2048], P('sp'), may hold values from -6 to 6
- query_in: bfloat16 [1536, 2048], P('sp', 'tp'), may hold values from -6 to 6
- value_in: bfloat16 [1536, 2048], P('sp', 'tp'), may hold values from -6 to 6
- forget_fwd: bfloat16 [1536, 2048], P('sp', 'tp'), may hold values from -4.5 to 4.5
- forget_bwd: bfloat16 [1536, 2048], P('sp', 'tp'), may hold values from -4.5 to 4.5
- jumps: float32 [16, 1536], P('tp', 'sp'), may hold values from -2.8 to 0
- gate_gap: float32 [2, 2048], P(None, 'tp'), may hold values from 0 to 0.1
- out_gate: bfloat16 [1536, 2048], P('sp', 'tp'), may hold values from -6 to 6
- head_gain: float32 [2048], P('tp'), may hold values from 0.1 to 1.9
- out_weight: bfloat16 [2048, 2048], P('tp'), may hold values from -0.25 to 0.25
- norm_gain: float32 [2048], replicated, may hold values from 0.1 to 1.9
- route_ids: int32 [1536, 4], P('sp'), may hold values from 0 to 31, all different within a row; in each aligned block of 192 rows (0 to 191, 192 to 383, ...) at most 36 rows name the same one
- route_weights: float32 [1536, 4], P('sp'), may hold values from 0.05 to 0.5
- w_gate: bfloat16 [32, 2048, 4096], P('sp', None, 'tp'), may hold values from -0.375 to 0.375
- w_up: bfloat16 [32, 2048, 4096], P('sp', None, 'tp'), may hold values from -0.375 to 0.375
- w_down: bfloat16 [32, 4096, 2048], P('sp', None, 'tp'), may hold values from -0.09375 to 0.09375
Outputs:
- mixed: bfloat16 [1536, 2048], P('sp', 'tp')
The draws below stay inside these ranges and needn't reach their ends.
Inputs may be any that keep to these rules, and one draw needn't show every extreme that they name: `route_ids`: in each aligned block of 192 rows each expert is named by at most 36 rows, and by exactly 36 in some block; each row names 4 different experts.
All inputs are finite; a program needn't handle non-finite values.
Results may differ from the reference program's by a relative error of at most 0.024.
Values may be sent and summed in bfloat16 or wider, within the bound.
A program may use at most 128 MiB of HBM per device.

```python
import math
import jax
import jax.numpy as jnp
import numpy as np
from jax import lax

HEADS = 16
HEAD_DIM = 128
D = 2048
FF = 4096
EXPERTS = 32
TOP = 4
TOK_SP = 192
TOKENS = 1536
CAP = 36
N_SP = 8
N_TP = 4


def draw_gate_gap(key, part):
    head_key, fast_key, slow_key = jax.random.split(jax.random.fold_in(key, 11), 3)
    fast_share = 0.5
    fast_heads = jax.random.uniform(head_key, (2, HEADS, 1), jnp.float32) < fast_share
    fast_gap = jax.random.uniform(fast_key, (2, HEADS, HEAD_DIM), jnp.float32, math.log(0.03), math.log(0.1))
    slow_gap = jax.random.uniform(slow_key, (2, HEADS, HEAD_DIM), jnp.float32, math.log(0.2), 0.0)
    gap_values = jnp.where(fast_heads, jnp.exp(fast_gap), jnp.exp(slow_gap) / TOKENS)
    return gap_values.reshape(2, D).astype(jnp.float32)


def forget_values(key):
    noise_key, level_key = jax.random.split(key)
    noise = jnp.clip(jax.random.normal(noise_key, (TOKENS, D), jnp.float32), -3.0, 3.0)
    levels = jax.random.uniform(level_key, (TOKENS // TOK_SP, 1, HEADS, 1), jnp.float32, -1.5, 1.5)
    shifted = noise.reshape(TOKENS // TOK_SP, TOK_SP, HEADS, HEAD_DIM) + levels
    return shifted.reshape(TOKENS, D).astype(jnp.bfloat16)


def draw_forget_fwd(key, part):
    return forget_values(jax.random.fold_in(key, 21))


def draw_forget_bwd(key, part):
    return forget_values(jax.random.fold_in(key, 22))


def draw_jumps(key, part):
    spot_key, size_key = jax.random.split(jax.random.fold_in(key, 31))
    spots = jax.random.randint(spot_key, (HEADS, 4), 0, TOKENS)
    sizes = jax.random.uniform(size_key, (HEADS, 4), jnp.float32, math.log(0.5), math.log(0.8))
    hits = jnp.arange(TOKENS, dtype=jnp.int32)[None, :, None] == spots[:, None, :]
    return jnp.sum(jnp.where(hits, sizes[:, None, :], 0.0), axis=2).astype(jnp.float32)


def block_scale(stream_key, shape, shards, smallest, high):
    loudness = 1.0
    for dim, blocks in shards:
        heights = jax.random.uniform(jax.random.fold_in(jax.random.fold_in(stream_key, 6), dim), (blocks,), jnp.float32, smallest / len(shards), high / len(shards))
        loudness = loudness * jnp.repeat(jnp.exp(heights), shape[dim] // blocks).reshape((-1,) + (1,) * (len(shape) - 1 - dim))
    return loudness


def shared_out(key, own, number, rows, number_of, top, limit, slope):
    ranking = jax.random.permutation(key, number_of)
    packed, common = shares(number_of, rows * top, limit, slope, True), shares(number_of, rows * top, limit, slope, False)
    places = jnp.arange(number_of)

    def named(tallies, turn):
        used = int((tallies > 0).sum())
        fixed = max(1, used // 4)
        moved = fixed + (places - fixed + turn * (used - fixed)) % max(1, number_of - fixed)
        return jnp.zeros((number_of,), jnp.int32).at[ranking[jnp.where(places < fixed, places, moved)]].set(jnp.asarray(tallies, jnp.int32))

    tallies = jnp.where(number % 4 == 0, named(packed, number // 4), named(common, number - number // 4 - 1))
    mixed = jax.random.permutation(jax.random.fold_in(own, 3), number_of)
    source_of, taker = mixed[0:number_of // 2 * 2:2], mixed[1:number_of // 2 * 2:2]
    slack = jnp.minimum(tallies[source_of] - 1, limit - tallies[taker]) // 2
    slack = jnp.where((source_of == ranking[0]) | (taker == ranking[0]) | (tallies[taker] == 0), 0, jnp.maximum(slack, 0))
    moved = jax.random.randint(jax.random.fold_in(own, 4), (number_of // 2,), 0, 1 << 20) % (slack + 1)
    tallies = tallies.at[source_of].add(-moved).at[taker].add(moved)
    labels = jnp.searchsorted(jnp.cumsum(tallies), jnp.arange(rows * top), side="right").astype(jnp.int32)
    grid = labels.reshape(top, rows).T
    grid = grid[jax.random.permutation(jax.random.fold_in(own, 1), rows)]
    turn = jax.random.randint(jax.random.fold_in(own, 2), (rows, 1), 0, top)
    return jnp.take_along_axis(grid, (jnp.arange(top)[None, :] + turn) % top, axis=1)


def shares(number_of, total, reach, lean, full):
    weights = [(1 << 20) // math.isqrt(grade ** lean) + 1 for grade in range(1, number_of + 1)]
    largest = reach if full else min(reach, max(-(-total // number_of), total * weights[0] // sum(weights)))
    least = 1 if total - largest >= number_of - 1 else 0
    counts, surplus = [largest] + [least] * (number_of - 1), total - largest - least * (number_of - 1)
    while surplus > 0:
        movable = [i for i in range(1, number_of) if counts[i] < largest] or [i for i in range(1, number_of) if counts[i] < reach]
        pool, left = sum([weights[i] for i in movable]), surplus
        for i in movable:
            extra = min(reach - counts[i], max(1, left * weights[i] // pool), surplus)
            counts[i] = counts[i] + extra
            surplus = surplus - extra
    return np.array(counts)


def scatter_about(stream_key, shape, scale, bound, pieces=(), held_as=jnp.bfloat16):
    entries = scale * jax.random.normal(stream_key, shape, jnp.float32)
    if pieces:
        entries = entries * block_scale(stream_key, shape, pieces, -0.22, 0.18)
    return jnp.clip(entries, -bound, bound).astype(held_as)


def setup_inputs(seed: int = 0) -> dict:
    streams_of = jax.random.split(jax.random.key(seed), 17)
    residual = scatter_about(streams_of[0], (TOKENS, D), 1.0, 6.0, ((0, 8),))
    query_in = scatter_about(streams_of[1], (TOKENS, D), 1.0, 6.0, ((0, 8), (1, 4)))
    value_in = scatter_about(streams_of[2], (TOKENS, D), 1.0, 6.0, ((0, 8), (1, 4)))
    forget_fwd = draw_forget_fwd(jax.random.fold_in(streams_of[16], 71), 0)
    forget_bwd = draw_forget_bwd(jax.random.fold_in(streams_of[16], 71), 0)
    jumps = draw_jumps(jax.random.fold_in(streams_of[16], 71), 0)
    gate_gap = draw_gate_gap(jax.random.fold_in(streams_of[16], 71), 0)
    out_gate = scatter_about(streams_of[7], (TOKENS, D), 1.0, 6.0, ((0, 8), (1, 4)))
    head_gain = jnp.clip(1.0 + 0.18 * jax.random.normal(streams_of[8], (D,), jnp.float32), 0.1, 1.9)
    out_weight = scatter_about(streams_of[9], (D, D), (D // 4) ** -0.5, 0.25, ((0, 4),))
    norm_gain = jnp.clip(1.0 + 0.18 * jax.random.normal(streams_of[10], (D,), jnp.float32), 0.1, 1.9)
    route_ids_keys = jax.random.split(jax.random.fold_in(streams_of[11], 1), TOKENS // TOK_SP)
    route_ids_turns = jax.random.permutation(jax.random.fold_in(streams_of[11], 3), TOKENS // TOK_SP)
    route_ids = jax.vmap(lambda own, number: shared_out(jax.random.fold_in(streams_of[11], 2), own, number, TOK_SP, EXPERTS, TOP, CAP, 1))(route_ids_keys, route_ids_turns).reshape((TOKENS, TOP))
    route_weights = jnp.clip(jnp.exp(math.log(0.5) - 2.3025851 * jax.random.uniform(streams_of[12], (TOKENS, TOP), jnp.float32) ** block_scale(streams_of[12], (TOKENS, TOP), ((0, 8),), -0.2, 0.2)), 0.05, 0.5)
    w_gate = scatter_about(streams_of[13], (EXPERTS, D, FF), (D // 8) ** -0.5, 0.375, ((0, 8), (2, 4)))
    w_up = scatter_about(streams_of[14], (EXPERTS, D, FF), (D // 8) ** -0.5, 0.375, ((0, 8), (2, 4)))
    w_down = scatter_about(streams_of[15], (EXPERTS, FF, D), FF ** -0.5, 0.09375, ((0, 8), (2, 4)))
    return dict(residual=residual, query_in=query_in, value_in=value_in, forget_fwd=forget_fwd, forget_bwd=forget_bwd, jumps=jumps, gate_gap=gate_gap, out_gate=out_gate, head_gain=head_gain, out_weight=out_weight, norm_gain=norm_gain, route_ids=route_ids, route_weights=route_weights, w_gate=w_gate, w_up=w_up, w_down=w_down)


highest_precision = lax.Precision.HIGHEST
eps_norm = 1e-06
limit_value = 7.0
alpha_value = 1.702

def recurrence(queries, keys_in, values, logs):

    def advance(current_state, step_items):
        current_query, key_now, value_now, log_now = step_items
        current_state = current_state * jnp.exp(log_now)[:, :, None] + key_now[:, :, None] * value_now[:, None, :]
        return (current_state, jnp.einsum('ob,obs->os', current_query, current_state, precision=highest_precision))
    zero_state = jnp.zeros((queries.shape[1], queries.shape[2], values.shape[2]), jnp.float32)
    unused, outputs = lax.scan(advance, zero_state, (queries, keys_in, values, logs))
    return outputs

def reference(residual, query_in, value_in, forget_fwd, forget_bwd, jumps, gate_gap, out_gate, head_gain, out_weight, norm_gain, route_ids, route_weights, w_gate, w_up, w_down):
    tokens, width = query_in.shape
    head_count = jumps.shape[0]
    head_width = width // head_count

    def by_head(array):
        return array.astype(jnp.float32).reshape(tokens, head_count, head_width)
    queries = jax.nn.silu(by_head(query_in))
    values = by_head(value_in)
    jump_rows = jnp.transpose(jumps)[:, :, None]

    def gate_terms(forget_in, gap):
        key_share = gap.reshape(head_count, head_width) * jax.nn.sigmoid(-by_head(forget_in))
        return (key_share, jnp.log1p(-key_share) + jump_rows)
    keys_fwd, logs_fwd = gate_terms(forget_fwd, gate_gap[0])
    keys_bwd, logs_bwd = gate_terms(forget_bwd, gate_gap[1])
    forward_out = recurrence(queries, keys_fwd, values, logs_fwd)
    backward_out = jnp.flip(recurrence(jnp.flip(queries, 0), jnp.flip(keys_bwd, 0), jnp.flip(values, 0), jnp.flip(logs_bwd, 0)), 0)
    mixed_heads = forward_out + backward_out
    mean_square = lax.optimization_barrier(jnp.mean(mixed_heads * mixed_heads, axis=-1, keepdims=True))
    normed = (mixed_heads * lax.rsqrt(mean_square + eps_norm)).reshape(tokens, width)
    gated = (normed * head_gain * jax.nn.silu(out_gate.astype(jnp.float32))).astype(jnp.bfloat16)
    group_width = width // N_TP
    gated_groups = jnp.transpose(gated.reshape(tokens, N_TP, group_width), (1, 0, 2))
    weight_groups = out_weight.reshape(N_TP, group_width, width)

    def add_group(total, group_items):
        term = jnp.dot(group_items[0], group_items[1], preferred_element_type=jnp.float32).astype(jnp.bfloat16)
        term = lax.optimization_barrier(term)
        return (total + term.astype(jnp.float32), None)
    summed, unused = lax.scan(add_group, jnp.zeros((tokens, width), jnp.float32), (gated_groups, weight_groups))
    stream = (residual.astype(jnp.float32) + summed).astype(jnp.bfloat16)
    stream_f = stream.astype(jnp.float32)
    row_scale = lax.rsqrt(lax.optimization_barrier(jnp.mean(stream_f * stream_f, axis=-1, keepdims=True)) + eps_norm)
    normed_rows = (stream_f * row_scale * norm_gain).astype(jnp.bfloat16)
    block = tokens // N_SP
    group_ids = route_ids.reshape(N_SP, block * TOP)
    one_hot = (group_ids[:, :, None] == jnp.arange(EXPERTS, dtype=jnp.int32)[None, None, :]).astype(jnp.int32)
    slot_rank = lax.optimization_barrier(jnp.sum((jnp.cumsum(one_hot, axis=1) - 1) * one_hot, axis=2))
    group_index = jnp.arange(N_SP, dtype=jnp.int32)[:, None]
    slot_index = (group_ids * (N_SP * CAP) + group_index * CAP + slot_rank).reshape(-1).astype(jnp.int32)
    owner_rows = (jnp.arange(tokens * TOP, dtype=jnp.int32) // TOP).astype(jnp.int32)
    slot_rows = jnp.full((EXPERTS * N_SP * CAP,), tokens, jnp.int32).at[slot_index].set(owner_rows)
    padded_rows = jnp.concatenate([normed_rows, jnp.zeros((1, width), jnp.bfloat16)], axis=0)

    def expert(expert_items):
        rows_index, gate_weight, up_weight, down_weight = expert_items
        rows = padded_rows[rows_index]
        gate_sum = jnp.minimum(jnp.dot(rows, gate_weight, preferred_element_type=jnp.float32), limit_value)
        up_sum = jnp.clip(jnp.dot(rows, up_weight, preferred_element_type=jnp.float32), -limit_value, limit_value)
        active = (gate_sum * jax.nn.sigmoid(alpha_value * gate_sum) * (up_sum + 1.0)).astype(jnp.bfloat16)
        return jnp.dot(active, down_weight, preferred_element_type=jnp.float32).astype(jnp.bfloat16)
    produced = lax.map(expert, (slot_rows.reshape(EXPERTS, N_SP * CAP), w_gate, w_up, w_down))
    picked = produced.reshape(EXPERTS * N_SP * CAP, width)[slot_index].astype(jnp.float32).reshape(tokens, TOP, width)
    moe_out = lax.optimization_barrier(jnp.sum(picked * route_weights[:, :, None], axis=1))
    return (stream_f + moe_out).astype(jnp.bfloat16)
```

```python
import functools
import math

import jax
import jax.numpy as jnp
from jax import lax
from jax.experimental import pallas as pl
from jax.experimental.pallas import tpu as pltpu
from jax.sharding import PartitionSpec as P

EXPERTS = 32
CAP = 36


highest_precision = lax.Precision.HIGHEST
eps_norm = 1e-06
limit_value = 7.0
alpha_value = 1.702


def entering(x, axis, join, neutral, backward):
    count = lax.axis_size(axis)
    place = lax.axis_index(axis)
    ahead = count - 1 - place if backward else place
    gathered = jax.tree.map(
        lambda a, kind: lax.all_gather(a.astype(kind), axis),
        x,
        jax.tree.map(lambda a: jnp.bfloat16 if a.dtype == jnp.float32 else a.dtype, x),
    )
    state = jax.tree.map(lambda a, e: jnp.zeros_like(a) + jnp.asarray(e, a.dtype), x, neutral)

    def one(hop, state):
        source = count - 1 - hop if backward else hop
        return join(
            state,
            jax.tree.map(
                lambda a, own: lax.dynamic_index_in_dim(a, source, 0, False).astype(own.dtype),
                gathered,
                x,
            ),
        )

    return lax.fori_loop(0, ahead, one, state)


def block_pass(queries, keys_in, values, logs):
    head_rows, head_count, head_width = queries.shape
    block_size = math.gcd(head_rows, 64)
    block_count = head_rows // block_size

    def to_blocks(array):
        return array.reshape(block_count, block_size, head_count, array.shape[-1])

    q_block, k_block, v_block, log_block = (
        to_blocks(queries),
        to_blocks(keys_in),
        to_blocks(values),
        to_blocks(logs),
    )
    decay_sums = jnp.cumsum(log_block, axis=1)
    middle = decay_sums[:, block_size // 2 - 1 : block_size // 2]
    scores = jnp.einsum(
        "nthk,nshk->nhts",
        q_block * jnp.exp(decay_sums - middle),
        k_block * jnp.exp(middle - decay_sums),
        precision=highest_precision,
    )
    lower_mask = jnp.tril(jnp.ones((block_size, block_size), bool))
    within = jnp.einsum(
        "nhts,nshv->nthv", jnp.where(lower_mask, scores, 0.0), v_block, precision=highest_precision
    )
    block_end = decay_sums[:, -1]
    q_start = q_block * jnp.exp(decay_sums)
    k_end = k_block * jnp.exp(block_end[:, None] - decay_sums)

    def advance(current_state, block_items):
        query_segment, key_segment, value_segment, decay_part = block_items
        state_readout = jnp.einsum(
            "qwe,wei->qwi", query_segment, current_state, precision=highest_precision
        )
        current_state = current_state * jnp.exp(decay_part)[:, :, None] + jnp.einsum(
            "foj,fox->ojx", key_segment, value_segment, precision=highest_precision
        )
        return (current_state, state_readout)

    zero_state = jnp.zeros((head_count, head_width, values.shape[-1]), jnp.float32)
    final_state, across = lax.scan(advance, zero_state, (q_start, k_end, v_block, block_end))
    return ((within + across).reshape(head_rows, head_count, -1), final_state)


def combine_states(first_part, second_part):
    return (
        first_part[0] * second_part[0],
        second_part[0][:, :, None] * first_part[1] + second_part[1],
    )


def carried(queries, logs, running_state):
    decayed_state = queries * jnp.exp(jnp.cumsum(logs, axis=0))
    return jnp.einsum("una,nae->une", decayed_state, running_state, precision=highest_precision)


def shards(
    residual,
    query_in,
    value_in,
    forget_fwd,
    forget_bwd,
    jumps,
    gate_gap,
    out_gate,
    head_gain,
    out_weight,
    norm_gain,
    route_ids,
    route_weights,
    w_gate,
    w_up,
    w_down,
):
    head_rows, local_width = query_in.shape
    head_count = jumps.shape[0]
    head_width = local_width // head_count

    def by_head(array):
        return array.astype(jnp.float32).reshape(head_rows, head_count, head_width)

    queries = jax.nn.silu(by_head(query_in))
    values = by_head(value_in)
    jump_rows = jnp.transpose(jumps)[:, :, None]

    def gate_terms(forget_in, gap):
        key_share = gap.reshape(head_count, head_width) * jax.nn.sigmoid(-by_head(forget_in))
        return (key_share, jnp.log1p(-key_share) + jump_rows)

    keys_fwd, logs_fwd = gate_terms(forget_fwd, gate_gap[0])
    keys_bwd, logs_bwd = gate_terms(forget_bwd, gate_gap[1])
    ones_part = jnp.ones((head_count, head_width), jnp.float32)
    zero_part = jnp.zeros((head_count, head_width, head_width), jnp.float32)
    local_fwd, final_fwd = block_pass(queries, keys_fwd, values, logs_fwd)
    summary_fwd = (jnp.exp(jnp.sum(logs_fwd, axis=0)), final_fwd)
    carry_fwd = entering(summary_fwd, "sp", combine_states, (ones_part, zero_part), False)[1]
    flip_queries = jnp.flip(queries, 0)
    flip_logs = jnp.flip(logs_bwd, 0)
    local_bwd, final_bwd = block_pass(
        flip_queries, jnp.flip(keys_bwd, 0), jnp.flip(values, 0), flip_logs
    )
    summary_bwd = (jnp.exp(jnp.sum(logs_bwd, axis=0)), final_bwd)
    carry_bwd = entering(summary_bwd, "sp", combine_states, (ones_part, zero_part), True)[1]
    forward_out = local_fwd + carried(queries, logs_fwd, carry_fwd)
    backward_out = jnp.flip(local_bwd + carried(flip_queries, flip_logs, carry_bwd), 0)
    mixed_heads = forward_out + backward_out
    mean_square = jnp.mean(mixed_heads * mixed_heads, axis=-1, keepdims=True)
    normed = (mixed_heads * lax.rsqrt(mean_square + eps_norm)).reshape(head_rows, local_width)
    gated = (normed * head_gain * jax.nn.silu(out_gate.astype(jnp.float32))).astype(jnp.bfloat16)
    head_terms = jnp.dot(gated, out_weight, preferred_element_type=jnp.float32)
    summed = lax.psum(head_terms.astype(jnp.bfloat16), "tp").astype(jnp.float32)
    stream = (residual.astype(jnp.float32) + summed).astype(jnp.bfloat16)
    stream_f = stream.astype(jnp.float32)
    row_scale = lax.rsqrt(jnp.mean(stream_f * stream_f, axis=-1, keepdims=True) + eps_norm)
    normed_rows = (stream_f * row_scale * norm_gain).astype(jnp.bfloat16)
    top_count = route_ids.shape[1]
    flat_ids = route_ids.reshape(-1)
    one_hot = (flat_ids[:, None] == jnp.arange(EXPERTS, dtype=jnp.int32)[None, :]).astype(jnp.int32)
    slot_rank = jnp.sum((jnp.cumsum(one_hot, axis=0) - 1) * one_hot, axis=1)
    slot_index = flat_ids * CAP + slot_rank
    owner_rows = jnp.arange(head_rows * top_count, dtype=jnp.int32) // top_count
    slot_rows = jnp.full((EXPERTS * CAP,), head_rows, jnp.int32).at[slot_index].set(owner_rows)
    padded_rows = jnp.concatenate(
        [normed_rows, jnp.zeros((1, normed_rows.shape[1]), jnp.bfloat16)], axis=0
    )
    tp_index = lax.axis_index("tp")
    part_width = w_down.shape[2]
    column_rows = lax.dynamic_slice_in_dim(padded_rows, tp_index * part_width, part_width, 1)
    buffer = column_rows[slot_rows].reshape(EXPERTS, CAP, part_width)
    arrived = lax.all_to_all(buffer, "sp", split_axis=0, concat_axis=1, tiled=True)
    piece = lax.all_gather(arrived, "tp", axis=2, tiled=True)
    gate_sum = jnp.einsum("esd,edf->esf", piece, w_gate, preferred_element_type=jnp.float32)
    up_sum = jnp.einsum("esd,edf->esf", piece, w_up, preferred_element_type=jnp.float32)
    gate_sum = jnp.minimum(gate_sum, limit_value)
    up_sum = jnp.clip(up_sum, -limit_value, limit_value)
    active = (gate_sum * jax.nn.sigmoid(alpha_value * gate_sum) * (up_sum + 1.0)).astype(
        jnp.bfloat16
    )
    produced = jnp.einsum(
        "esf,efd->esd",
        lax.all_gather(active, "tp", axis=2, tiled=True),
        w_down,
        preferred_element_type=jnp.float32,
    ).astype(jnp.bfloat16)
    returned = lax.all_to_all(produced, "sp", split_axis=1, concat_axis=0, tiled=True)
    picked = returned.reshape(EXPERTS * CAP, part_width)[slot_index].astype(jnp.float32)
    picked = picked.reshape(head_rows, top_count, part_width)
    moe_out = jnp.sum(picked * route_weights[:, :, None], axis=1)
    own_columns = lax.dynamic_slice_in_dim(stream_f, tp_index * part_width, part_width, 1)
    return (own_columns + moe_out).astype(jnp.bfloat16)


MESH = pl.DeviceIdType.MESH
f32 = jnp.float32
bf16 = jnp.bfloat16
SLOT_PAD = 48


def mm(a, b, dims=((1,), (0,))):
    return lax.dot_general(a.astype(bf16), b.astype(bf16), (dims, ((), ())), preferred_element_type=f32)


def mm_exact(a, b, dims=((1,), (0,))):
    return lax.dot_general(
        a.astype(f32), b.astype(f32), (dims, ((), ())), precision=highest_precision, preferred_element_type=f32
    )


def remote(src, dst, send, recv, device):
    return pltpu.make_async_remote_copy(
        src_ref=src, dst_ref=dst, send_sem=send, recv_sem=recv, device_id=device, device_id_type=MESH
    )


def greet(devices):
    barrier = pltpu.get_barrier_semaphore()
    for device in devices:
        pl.semaphore_signal(barrier, inc=1, device_id=device, device_id_type=MESH)
    pl.semaphore_wait(barrier, len(devices))


def front_kernel(
    n_sp,
    n_tp,
    ids_ref,
    query_ref,
    value_ref,
    ff_ref,
    fb_ref,
    jumps_ref,
    gap_ref,
    og_ref,
    hg_ref,
    ow_ref,
    res_ref,
    ng_ref,
    xs_ref,
    stream_ref,
    dslot_ref,
    st,
    dec,
    rst,
    rdec,
    pos,
    rpos,
    gated,
    oacc,
    qcarry,
    pb,
    rpb,
    sq,
    rsq,
    rows,
    st_send,
    st_recv,
    dec_send,
    dec_recv,
    pos_send,
    pos_recv,
    rs_send,
    rs_recv,
    sq_send,
    sq_recv,
    ag_send,
    ag_recv,
):
    p = lax.axis_index("sp")
    t = lax.axis_index("tp")
    n, width = query_ref.shape
    heads = jumps_ref.shape[0]
    hw = width // heads
    n_exp = EXPERTS // n_sp
    n_z = n_sp // 2
    group = xs_ref.shape[1] // (2 * CAP)
    partner = p + 1 - 2 * lax.rem(p, 2)
    zpeers = [lax.rem(p + 2 * k, n_sp) for k in range(1, n_z)]
    zfrom = [lax.rem(p + n_sp - 2 * k, n_sp) for k in range(1, n_z)]
    speers = [lax.rem(p + k, n_sp) for k in range(1, n_sp)]
    tpeers = [lax.rem(t + k, n_tp) for k in range(1, n_tp)]
    tfrom = [lax.rem(t + n_tp - k, n_tp) for k in range(1, n_tp)]
    greet([(s, t) for s in speers] + [(p, u) for u in tpeers])

    row_i = lax.broadcasted_iota(jnp.int32, (n, n), 0)
    col_i = lax.broadcasted_iota(jnp.int32, (n, n), 1)
    lower = (col_i <= row_i).astype(f32)
    upper = (col_i >= row_i).astype(f32)
    eye = (col_i == row_i).astype(f32)

    ex_i = lax.broadcasted_iota(jnp.int32, (n, EXPERTS), 1)
    picks = [(ids_ref[:, j : j + 1] == ex_i).astype(f32) for j in range(ids_ref.shape[1])]
    named = sum(picks)
    strict_before = (row_i < col_i).astype(f32)
    named_t = mm(named, eye, ((0,), (0,)))
    rank_t = mm(named, strict_before, ((0,), (0,)))
    place = lax.rem(p, group).astype(f32) * CAP
    table = jnp.where(named_t > 0.5, rank_t + place, -1.0)
    pos[...] = jnp.full(pos.shape, -1.0, f32)
    for d in range(n_sp):
        pos[d, 0:n_exp, :] = table[d * n_exp : (d + 1) * n_exp, :]
    rank = mm(col_i < row_i, named)
    base = ex_i.astype(f32) * SLOT_PAD + rank
    lane = lax.broadcasted_iota(jnp.int32, dslot_ref.shape, 1)
    slots = jnp.zeros(dslot_ref.shape, f32)
    for j, pick in enumerate(picks):
        slots = jnp.where(lane == j, jnp.sum(pick * base, axis=1, keepdims=True), slots)
    dslot_ref[...] = slots

    def gates(ref, index):
        key = gap_ref[index : index + 1, :] * jax.nn.sigmoid(-ref[...].astype(f32))
        return key, jnp.log1p(-key)

    key_f, log_f = gates(ff_ref, 0)
    key_b, log_b = gates(fb_ref, 1)
    sum_f = mm_exact(lower, log_f)
    sum_b = mm_exact(upper, log_b)
    jcol_f = mm_exact(lower, jumps_ref[...], ((1,), (1,)))
    jcol_b = mm_exact(upper, jumps_ref[...], ((1,), (1,)))
    jrow_f = mm_exact(jumps_ref[...], lower, ((1,), (1,)))
    jrow_b = mm_exact(jumps_ref[...], upper, ((1,), (1,)))
    query = query_ref[...].astype(f32)
    query = query * jax.nn.sigmoid(query)
    end_f, end_b = sum_f[n - 1 : n, :], sum_b[0:1, :]
    for h in range(heads):
        cols = slice(h * hw, (h + 1) * hw)
        for d, (key, total, end, jcol, jend) in enumerate(
            (
                (key_f, sum_f, end_f, jcol_f, n - 1),
                (key_b, sum_b, end_b, jcol_b, 0),
            )
        ):
            jtot = jcol[jend : jend + 1, h : h + 1]
            decay = jnp.exp(jnp.minimum(end[:, cols] - total[:, cols] + (jtot - jcol[:, h : h + 1]), 0.0))
            st[d, h * hw : (h + 1) * hw, :] = mm(
                value_ref[:, cols], key[:, cols] * decay, ((0,), (0,))
            ).astype(bf16)
            dec[d, :, cols] = jnp.broadcast_to(jnp.exp(end[:, cols] + jtot), (dec.shape[1], hw))
            qcarry[d, :, cols] = (
                query[:, cols] * jnp.exp(total[:, cols] + jcol[:, h : h + 1])
            ).astype(bf16)

    pending = []

    def go(copy):
        copy.start()
        pending.append(copy)

    st_next = 0
    for peer in [partner] + zpeers:
        way = jnp.where(peer > p, 0, 1)
        go(remote(st.at[way], rst.at[p], st_send.at[st_next], st_recv.at[p], (peer, t)))
        go(remote(dec.at[way], rdec.at[p], dec_send.at[st_next], dec_recv.at[p], (peer, t)))
        st_next += 1
    for i, peer in enumerate(speers):
        go(remote(pos.at[peer], rpos.at[p], pos_send.at[i], pos_recv.at[p], (peer, t)))

    mid_f, mid_b = sum_f[n // 2 : n // 2 + 1, :], sum_b[n // 2 : n // 2 + 1, :]
    q_f, k_f = query * jnp.exp(sum_f - mid_f), key_f * jnp.exp(mid_f - sum_f)
    q_b, k_b = query * jnp.exp(sum_b - mid_b), key_b * jnp.exp(mid_b - sum_b)
    for h in range(heads):
        cols = slice(h * hw, (h + 1) * hw)
        jump_f = jnp.exp(jnp.minimum(jcol_f[:, h : h + 1] - jrow_f[h : h + 1, :], 0.0))
        jump_b = jnp.exp(jnp.minimum(jcol_b[:, h : h + 1] - jrow_b[h : h + 1, :], 0.0))
        score = mm(q_f[:, cols], k_f[:, cols], ((1,), (1,))) * (jump_f * lower)
        score += mm(q_b[:, cols], k_b[:, cols], ((1,), (1,))) * (jump_b * upper)
        oacc[:, cols] = mm(score, value_ref[:, cols])

    def st_wait(source):
        remote(st.at[0], rst.at[source], st_send.at[0], st_recv.at[source], (partner, t)).wait_recv()
        remote(dec.at[0], rdec.at[source], dec_send.at[0], dec_recv.at[source], (partner, t)).wait_recv()

    for source in zfrom:
        st_wait(source)
        go(remote(rst.at[source], rst.at[source], st_send.at[st_next], st_recv.at[source], (partner, t)))
        go(remote(rdec.at[source], rdec.at[source], dec_send.at[st_next], dec_recv.at[source], (partner, t)))
        st_next += 1
    st_wait(partner)
    for source in zfrom:
        st_wait(source + 1 - 2 * lax.rem(p, 2))

    def carry_from(first, step, count, d):
        def one(hop, states):
            source = first + step * hop
            return tuple(
                rdec[source, 0:1, h * hw : (h + 1) * hw] * states[h]
                + rst[source, h * hw : (h + 1) * hw, :].astype(f32)
                for h in range(heads)
            )

        states = lax.fori_loop(0, count, one, tuple(jnp.zeros((hw, hw), f32) for h in range(heads)))
        for h in range(heads):
            cols = slice(h * hw, (h + 1) * hw)
            oacc[:, cols] += mm(qcarry[d, :, cols], states[h], ((1,), (1,)))

    carry_from(0, 1, p, 0)
    carry_from(n_sp - 1, -1, n_sp - 1 - p, 1)

    for h in range(heads):
        cols = slice(h * hw, (h + 1) * hw)
        out = oacc[:, cols]
        scale = lax.rsqrt(jnp.mean(out * out, axis=-1, keepdims=True) + eps_norm)
        gate = og_ref[:, cols].astype(f32)
        gated[:, cols] = (out * scale * hg_ref[:, cols] * (gate * jax.nn.sigmoid(gate))).astype(bf16)

    for u in range(n_tp):
        pb[u] = mm(gated[...], ow_ref[:, u * width : (u + 1) * width]).astype(bf16)
    for i, peer in enumerate(tpeers):
        go(remote(pb.at[peer], rpb.at[t], rs_send.at[i], rs_recv.at[t], (p, peer)))
    own = pl.ds(pl.multiple_of(t * width, 128), width)
    total = pb[t].astype(f32)
    for source in tfrom:
        remote(pb.at[0], rpb.at[source], rs_send.at[0], rs_recv.at[source], (p, tpeers[0])).wait_recv()
        total = total + rpb[source].astype(f32)
    stream = (res_ref[:, own].astype(f32) + total).astype(bf16)
    stream_ref[...] = stream
    stream = stream.astype(f32)
    sq[...] = mm_exact(jnp.ones((sq.shape[0], width), f32), stream * stream, ((1,), (1,)))
    for i, peer in enumerate(tpeers):
        go(remote(sq, rsq.at[t], sq_send.at[i], sq_recv.at[t], (p, peer)))
    squares = sq[...]
    for source in tfrom:
        remote(sq, rsq.at[source], sq_send.at[0], sq_recv.at[source], (p, tpeers[0])).wait_recv()
        squares = squares + rsq[source]
    scale = lax.rsqrt(squares / (width * n_tp) + eps_norm)
    scale = mm_exact(eye, scale, ((1,), (1,)))[:, 0:1]
    rows[p, t] = (stream * scale * ng_ref[:, own]).astype(bf16)

    ag_next = 0

    def spread(block, share, device):
        nonlocal ag_next
        go(
            remote(
                rows.at[block, share],
                rows.at[block, share],
                ag_send.at[ag_next],
                ag_recv.at[block, share],
                device,
            )
        )
        ag_next += 1

    def arrive(block, share):
        remote(
            rows.at[block, share],
            rows.at[block, share],
            ag_send.at[0],
            ag_recv.at[block, share],
            (partner, t),
        ).wait_recv()

    for peer in zpeers:
        spread(p, t, (peer, t))
    for peer in tpeers:
        spread(p, t, (p, peer))
    spread(p, t, (partner, t))
    for block in zfrom:
        arrive(block, t)
        for peer in tpeers:
            spread(block, t, (p, peer))
        spread(block, t, (partner, t))
    for block in [p] + zfrom:
        for share in tfrom:
            arrive(block, share)
            spread(block, share, (partner, t))
    for source in speers:
        remote(pos.at[0], rpos.at[source], pos_send.at[0], pos_recv.at[source], (partner, t)).wait_recv()
    rpos[p] = pos[p]
    for block in [p] + zfrom:
        other = block + 1 - 2 * lax.rem(p, 2)
        arrive(other, t)
        for share in tfrom:
            arrive(other, share)

    half = group * CAP
    slot_i = lax.broadcasted_iota(jnp.int32, (half, n), 0).astype(f32)
    for e in range(n_exp):
        for g in range(n_sp // group):
            hot = [(slot_i == rpos[g * group + b, e : e + 1, :]).astype(bf16) for b in range(group)]

            def one(u, unused, hot=hot, g=g, e=e):
                part = mm(hot[0], rows[g * group, u])
                for b in range(1, group):
                    part = part + mm(hot[b], rows[g * group + b, u])
                xs_ref[
                    e, g * half : (g + 1) * half, pl.ds(pl.multiple_of(u * width, 128), width)
                ] = part.astype(bf16)
                return unused

            lax.fori_loop(0, n_tp, one, 0)
    for copy in pending:
        copy.wait_send()


def expert_kernel(
    n_sp,
    n_tp,
    xs_ref,
    wg_ref,
    wu_ref,
    wd_ref,
    stream_ref,
    dslot_ref,
    rw_ref,
    out_ref,
    gbuf,
    ubuf,
    wd,
    acts,
    prod,
    rprod,
    wsem,
    dsem,
    act_send,
    act_recv,
    ret_send,
    ret_recv,
):
    p = lax.axis_index("sp")
    t = lax.axis_index("tp")
    n_exp, depth, hidden = wg_ref.shape
    slots = xs_ref.shape[1]
    tile = gbuf.shape[2]
    tiles = hidden // tile
    xn = t + 1 - 2 * lax.rem(t, 2)
    yn = lax.rem(t + 2, n_tp)
    dg = n_tp - 1 - t
    speers = [lax.rem(p + k, n_sp) for k in range(1, n_sp)]
    half = slots // 2
    halves = (pl.ds(0, half), pl.ds(half, half))

    def fetch(step, slot):
        e, i = step // tiles, lax.rem(step, tiles)
        cols = pl.ds(pl.multiple_of(i * tile, 128), tile)
        return (
            pltpu.make_async_copy(wg_ref.at[e, :, cols], gbuf.at[slot], wsem.at[0, slot]),
            pltpu.make_async_copy(wu_ref.at[e, :, cols], ubuf.at[slot], wsem.at[1, slot]),
        )

    for step in range(2):
        for copy in fetch(step, step):
            copy.start()
    down = [pltpu.make_async_copy(wd_ref.at[e], wd.at[e], dsem.at[e]) for e in range(n_exp)]
    greet([(s, t) for s in speers] + [(p, xn), (p, yn)])
    prod[...] = jnp.zeros(prod.shape, bf16)

    def act_copy(e, block, part, number, device):
        ref = acts.at[e, block, halves[part]]
        return remote(ref, ref, act_send.at[e, number], act_recv.at[e, block, part], (p, device))

    def own_sends(e):
        return (
            act_copy(e, t, 0, 0, xn),
            act_copy(e, t, 1, 1, yn),
            act_copy(e, t, 1, 2, xn),
            act_copy(e, t, 0, 3, yn),
        )

    def expert(e, unused):
        def part(i, unused):
            step = e * tiles + i
            slot = lax.rem(step, 2)
            for copy in fetch(step, slot):
                copy.wait()
            x = xs_ref[e]
            gate = jnp.dot(x, gbuf[slot], preferred_element_type=f32)
            up = jnp.dot(x, ubuf[slot], preferred_element_type=f32)
            gate = jnp.minimum(gate, limit_value)
            up = jnp.clip(up, -limit_value, limit_value)
            cols = pl.ds(pl.multiple_of(i * tile, 128), tile)
            acts[e, t, :, cols] = (gate * jax.nn.sigmoid(alpha_value * gate) * (up + 1.0)).astype(bf16)

            @pl.when(step + 2 < n_exp * tiles)
            def _():
                for copy in fetch(step + 2, slot):
                    copy.start()

            return unused

        lax.fori_loop(0, tiles, part, 0)
        for copy in own_sends(e):
            copy.start()
        return unused

    lax.fori_loop(0, n_exp, expert, 0)
    for copy in down:
        copy.start()

    def forward(e, unused):
        act_copy(e, xn, 0, 0, xn).wait_recv()
        act_copy(e, xn, 0, 4, yn).start()
        act_copy(e, yn, 1, 0, xn).wait_recv()
        act_copy(e, yn, 1, 5, xn).start()
        return unused

    lax.fori_loop(0, n_exp, forward, 0)
    for copy in down:
        copy.wait()

    def ret_copy(e, i, peer):
        return remote(prod.at[e, peer], rprod.at[p, e], ret_send.at[e, i], ret_recv.at[e, p], (peer, t))

    def lower(e, unused):
        act_copy(e, xn, 1, 0, xn).wait_recv()
        act_copy(e, yn, 0, 0, xn).wait_recv()
        act_copy(e, dg, 0, 0, xn).wait_recv()
        act_copy(e, dg, 1, 0, xn).wait_recv()
        total = jnp.dot(acts[e, 0], wd[e, 0:hidden, :], preferred_element_type=f32)
        for u in range(1, n_tp):
            total += jnp.dot(acts[e, u], wd[e, u * hidden : (u + 1) * hidden, :], preferred_element_type=f32)
        for s in range(n_sp):
            prod[e, s, 0:CAP, :] = total[s * CAP : (s + 1) * CAP, :].astype(bf16)
        for i, peer in enumerate(speers):
            ret_copy(e, i, peer).start()
        rprod[p, e] = prod[e, p]
        return unused

    lax.fori_loop(0, n_exp, lower, 0)

    tokens, width = stream_ref.shape
    total = stream_ref[...].astype(f32)
    lane = lax.broadcasted_iota(jnp.int32, (tokens, n_exp * SLOT_PAD), 1).astype(f32)

    def returns(k, total):
        source = lax.rem(p + n_sp - k, n_sp)

        @pl.when(k > 0)
        def _():
            for e in range(n_exp):
                remote(
                    prod.at[e, 0], rprod.at[source, e], ret_send.at[e, 0], ret_recv.at[e, source], (speers[0], t)
                ).wait_recv()

        first = (source * (n_exp * SLOT_PAD)).astype(f32)
        mix = jnp.zeros(lane.shape, f32)
        for j in range(rw_ref.shape[1]):
            mix += jnp.where(dslot_ref[:, j : j + 1] - first == lane, rw_ref[:, j : j + 1], 0.0)
        high = mix.astype(bf16)
        low = (mix - high.astype(f32)).astype(bf16)
        block = rprod[source].reshape(n_exp * SLOT_PAD, width)
        return (
            total
            + jnp.dot(high, block, preferred_element_type=f32)
            + jnp.dot(low, block, preferred_element_type=f32)
        )

    total = lax.fori_loop(0, n_sp, returns, total)
    out_ref[...] = total.astype(bf16)

    def drain(e, unused):
        for copy in own_sends(e):
            copy.wait_send()
        act_copy(e, xn, 0, 4, yn).wait_send()
        act_copy(e, yn, 1, 5, xn).wait_send()
        for i, peer in enumerate(speers):
            ret_copy(e, i, peer).wait_send()
        return unused

    lax.fori_loop(0, n_exp, drain, 0)


def fused(
    n_sp,
    n_tp,
    residual,
    query_in,
    value_in,
    forget_fwd,
    forget_bwd,
    jumps,
    gate_gap,
    out_gate,
    head_gain,
    out_weight,
    norm_gain,
    route_ids,
    route_weights,
    w_gate,
    w_up,
    w_down,
):
    tokens, width = query_in.shape
    heads = jumps.shape[0]
    hw = width // heads
    n_exp, model, hidden = w_gate.shape
    slots = n_sp * CAP
    vmem = pl.BlockSpec(memory_space=pltpu.VMEM)
    dma = pltpu.SemaphoreType.DMA
    group = n_sp // 2
    n_ag = (n_sp // 2) * n_tp * 2
    xs, stream, dslot = pl.pallas_call(
        functools.partial(front_kernel, n_sp, n_tp),
        out_shape=(
            jax.ShapeDtypeStruct((n_exp, slots, model), bf16),
            jax.ShapeDtypeStruct((tokens, width), bf16),
            jax.ShapeDtypeStruct((tokens, 128), f32),
        ),
        in_specs=[vmem] * 12,
        out_specs=(vmem, vmem, vmem),
        scratch_shapes=[
            pltpu.VMEM((2, heads * hw, hw), bf16),
            pltpu.VMEM((2, 8, width), f32),
            pltpu.VMEM((n_sp, heads * hw, hw), bf16),
            pltpu.VMEM((n_sp, 8, width), f32),
            pltpu.VMEM((n_sp, 8, tokens), f32),
            pltpu.VMEM((n_sp, 8, tokens), f32),
            pltpu.VMEM((tokens, width), bf16),
            pltpu.VMEM((tokens, width), f32),
            pltpu.VMEM((2, tokens, width), bf16),
            pltpu.VMEM((n_tp, tokens, width), bf16),
            pltpu.VMEM((n_tp, tokens, width), bf16),
            pltpu.VMEM((8, tokens), f32),
            pltpu.VMEM((n_tp, 8, tokens), f32),
            pltpu.VMEM((n_sp, n_tp, tokens, width), bf16),
            dma((n_sp,)),
            dma((n_sp,)),
            dma((n_sp,)),
            dma((n_sp,)),
            dma((n_sp,)),
            dma((n_sp,)),
            dma((n_tp,)),
            dma((n_tp,)),
            dma((n_tp,)),
            dma((n_tp,)),
            dma((n_ag,)),
            dma((n_sp, n_tp)),
        ],
        compiler_params=pltpu.CompilerParams(
            collective_id=0, has_side_effects=True, vmem_limit_bytes=48 * 1024 * 1024
        ),
        name="front",
    )(
        route_ids,
        query_in,
        value_in,
        forget_fwd,
        forget_bwd,
        jumps,
        gate_gap,
        out_gate,
        head_gain.reshape(1, width),
        out_weight,
        residual,
        norm_gain.reshape(1, model),
    )
    tile = math.gcd(hidden, 512)
    anywhere = pl.BlockSpec(memory_space=pl.ANY)
    return pl.pallas_call(
        functools.partial(expert_kernel, n_sp, n_tp),
        out_shape=jax.ShapeDtypeStruct((tokens, width), bf16),
        in_specs=[vmem, anywhere, anywhere, anywhere, vmem, vmem, vmem],
        out_specs=vmem,
        scratch_shapes=[
            pltpu.VMEM((2, model, tile), bf16),
            pltpu.VMEM((2, model, tile), bf16),
            pltpu.VMEM((n_exp, hidden * n_tp, width), bf16),
            pltpu.VMEM((n_exp, n_tp, slots, hidden), bf16),
            pltpu.VMEM((n_exp, n_sp, SLOT_PAD, width), bf16),
            pltpu.VMEM((n_sp, n_exp, SLOT_PAD, width), bf16),
            dma((2, 2)),
            dma((n_exp,)),
            dma((n_exp, 6)),
            dma((n_exp, n_tp, 2)),
            dma((n_exp, n_sp)),
            dma((n_exp, n_sp)),
        ],
        compiler_params=pltpu.CompilerParams(
            collective_id=1, has_side_effects=True, vmem_limit_bytes=60 * 1024 * 1024
        ),
        name="experts",
    )(xs, w_gate, w_up, w_down, stream, dslot, route_weights)


def solution(mesh):
    n_sp, n_tp = mesh.shape["sp"], mesh.shape["tp"]
    square = n_tp == 4 and n_sp % 2 == 0 and n_sp <= 8
    program = functools.partial(fused, n_sp, n_tp) if square else shards

    return jax.shard_map(
        program,
        mesh=mesh,
        in_specs=(
            P("sp", None),
            P("sp", "tp"),
            P("sp", "tp"),
            P("sp", "tp"),
            P("sp", "tp"),
            P("tp", "sp"),
            P(None, "tp"),
            P("sp", "tp"),
            P("tp"),
            P("tp", None),
            P(),
            P("sp", None),
            P("sp", None),
            P("sp", None, "tp"),
            P("sp", None, "tp"),
            P("sp", None, "tp"),
        ),
        out_specs=P("sp", "tp"),
        check_vma=False,
    )
```

```python
import functools
import math

import jax
import jax.numpy as jnp
from jax import lax
from jax.experimental import pallas as pl
from jax.experimental.pallas import tpu as pltpu
from jax.sharding import PartitionSpec as P

EXPERTS = 32
CAP = 36


highest_precision = lax.Precision.HIGHEST
eps_norm = 1e-06
limit_value = 7.0
alpha_value = 1.702


def entering(x, axis, join, neutral, backward):
    count = lax.axis_size(axis)
    place = lax.axis_index(axis)
    ahead = count - 1 - place if backward else place
    gathered = jax.tree.map(
        lambda a, kind: lax.all_gather(a.astype(kind), axis),
        x,
        jax.tree.map(lambda a: jnp.bfloat16 if a.dtype == jnp.float32 else a.dtype, x),
    )
    state = jax.tree.map(lambda a, e: jnp.zeros_like(a) + jnp.asarray(e, a.dtype), x, neutral)

    def one(hop, state):
        source = count - 1 - hop if backward else hop
        return join(
            state,
            jax.tree.map(
                lambda a, own: lax.dynamic_index_in_dim(a, source, 0, False).astype(own.dtype),
                gathered,
                x,
            ),
        )

    return lax.fori_loop(0, ahead, one, state)


def block_pass(queries, keys_in, values, logs):
    head_rows, head_count, head_width = queries.shape
    block_size = math.gcd(head_rows, 64)
    block_count = head_rows // block_size

    def to_blocks(array):
        return array.reshape(block_count, block_size, head_count, array.shape[-1])

    q_block, k_block, v_block, log_block = (
        to_blocks(queries),
        to_blocks(keys_in),
        to_blocks(values),
        to_blocks(logs),
    )
    decay_sums = jnp.cumsum(log_block, axis=1)
    middle = decay_sums[:, block_size // 2 - 1 : block_size // 2]
    scores = jnp.einsum(
        "nthk,nshk->nhts",
        q_block * jnp.exp(decay_sums - middle),
        k_block * jnp.exp(middle - decay_sums),
        precision=highest_precision,
    )
    lower_mask = jnp.tril(jnp.ones((block_size, block_size), bool))
    within = jnp.einsum(
        "nhts,nshv->nthv", jnp.where(lower_mask, scores, 0.0), v_block, precision=highest_precision
    )
    block_end = decay_sums[:, -1]
    q_start = q_block * jnp.exp(decay_sums)
    k_end = k_block * jnp.exp(block_end[:, None] - decay_sums)

    def advance(current_state, block_items):
        query_segment, key_segment, value_segment, decay_part = block_items
        state_readout = jnp.einsum(
            "qwe,wei->qwi", query_segment, current_state, precision=highest_precision
        )
        current_state = current_state * jnp.exp(decay_part)[:, :, None] + jnp.einsum(
            "foj,fox->ojx", key_segment, value_segment, precision=highest_precision
        )
        return (current_state, state_readout)

    zero_state = jnp.zeros((head_count, head_width, values.shape[-1]), jnp.float32)
    final_state, across = lax.scan(advance, zero_state, (q_start, k_end, v_block, block_end))
    return ((within + across).reshape(head_rows, head_count, -1), final_state)


def combine_states(first_part, second_part):
    return (
        first_part[0] * second_part[0],
        second_part[0][:, :, None] * first_part[1] + second_part[1],
    )


def carried(queries, logs, running_state):
    decayed_state = queries * jnp.exp(jnp.cumsum(logs, axis=0))
    return jnp.einsum("una,nae->une", decayed_state, running_state, precision=highest_precision)


def shards(
    residual,
    query_in,
    value_in,
    forget_fwd,
    forget_bwd,
    jumps,
    gate_gap,
    out_gate,
    head_gain,
    out_weight,
    norm_gain,
    route_ids,
    route_weights,
    w_gate,
    w_up,
    w_down,
):
    head_rows, local_width = query_in.shape
    head_count = jumps.shape[0]
    head_width = local_width // head_count

    def by_head(array):
        return array.astype(jnp.float32).reshape(head_rows, head_count, head_width)

    queries = jax.nn.silu(by_head(query_in))
    values = by_head(value_in)
    jump_rows = jnp.transpose(jumps)[:, :, None]

    def gate_terms(forget_in, gap):
        key_share = gap.reshape(head_count, head_width) * jax.nn.sigmoid(-by_head(forget_in))
        return (key_share, jnp.log1p(-key_share) + jump_rows)

    keys_fwd, logs_fwd = gate_terms(forget_fwd, gate_gap[0])
    keys_bwd, logs_bwd = gate_terms(forget_bwd, gate_gap[1])
    ones_part = jnp.ones((head_count, head_width), jnp.float32)
    zero_part = jnp.zeros((head_count, head_width, head_width), jnp.float32)
    local_fwd, final_fwd = block_pass(queries, keys_fwd, values, logs_fwd)
    summary_fwd = (jnp.exp(jnp.sum(logs_fwd, axis=0)), final_fwd)
    carry_fwd = entering(summary_fwd, "sp", combine_states, (ones_part, zero_part), False)[1]
    flip_queries = jnp.flip(queries, 0)
    flip_logs = jnp.flip(logs_bwd, 0)
    local_bwd, final_bwd = block_pass(
        flip_queries, jnp.flip(keys_bwd, 0), jnp.flip(values, 0), flip_logs
    )
    summary_bwd = (jnp.exp(jnp.sum(logs_bwd, axis=0)), final_bwd)
    carry_bwd = entering(summary_bwd, "sp", combine_states, (ones_part, zero_part), True)[1]
    forward_out = local_fwd + carried(queries, logs_fwd, carry_fwd)
    backward_out = jnp.flip(local_bwd + carried(flip_queries, flip_logs, carry_bwd), 0)
    mixed_heads = forward_out + backward_out
    mean_square = jnp.mean(mixed_heads * mixed_heads, axis=-1, keepdims=True)
    normed = (mixed_heads * lax.rsqrt(mean_square + eps_norm)).reshape(head_rows, local_width)
    gated = (normed * head_gain * jax.nn.silu(out_gate.astype(jnp.float32))).astype(jnp.bfloat16)
    head_terms = jnp.dot(gated, out_weight, preferred_element_type=jnp.float32)
    summed = lax.psum(head_terms.astype(jnp.bfloat16), "tp").astype(jnp.float32)
    stream = (residual.astype(jnp.float32) + summed).astype(jnp.bfloat16)
    stream_f = stream.astype(jnp.float32)
    row_scale = lax.rsqrt(jnp.mean(stream_f * stream_f, axis=-1, keepdims=True) + eps_norm)
    normed_rows = (stream_f * row_scale * norm_gain).astype(jnp.bfloat16)
    top_count = route_ids.shape[1]
    flat_ids = route_ids.reshape(-1)
    one_hot = (flat_ids[:, None] == jnp.arange(EXPERTS, dtype=jnp.int32)[None, :]).astype(jnp.int32)
    slot_rank = jnp.sum((jnp.cumsum(one_hot, axis=0) - 1) * one_hot, axis=1)
    slot_index = flat_ids * CAP + slot_rank
    owner_rows = jnp.arange(head_rows * top_count, dtype=jnp.int32) // top_count
    slot_rows = jnp.full((EXPERTS * CAP,), head_rows, jnp.int32).at[slot_index].set(owner_rows)
    padded_rows = jnp.concatenate(
        [normed_rows, jnp.zeros((1, normed_rows.shape[1]), jnp.bfloat16)], axis=0
    )
    tp_index = lax.axis_index("tp")
    part_width = w_down.shape[2]
    column_rows = lax.dynamic_slice_in_dim(padded_rows, tp_index * part_width, part_width, 1)
    buffer = column_rows[slot_rows].reshape(EXPERTS, CAP, part_width)
    arrived = lax.all_to_all(buffer, "sp", split_axis=0, concat_axis=1, tiled=True)
    piece = lax.all_gather(arrived, "tp", axis=2, tiled=True)
    gate_sum = jnp.einsum("esd,edf->esf", piece, w_gate, preferred_element_type=jnp.float32)
    up_sum = jnp.einsum("esd,edf->esf", piece, w_up, preferred_element_type=jnp.float32)
    gate_sum = jnp.minimum(gate_sum, limit_value)
    up_sum = jnp.clip(up_sum, -limit_value, limit_value)
    active = (gate_sum * jax.nn.sigmoid(alpha_value * gate_sum) * (up_sum + 1.0)).astype(
        jnp.bfloat16
    )
    produced = jnp.einsum(
        "esf,efd->esd",
        lax.all_gather(active, "tp", axis=2, tiled=True),
        w_down,
        preferred_element_type=jnp.float32,
    ).astype(jnp.bfloat16)
    returned = lax.all_to_all(produced, "sp", split_axis=1, concat_axis=0, tiled=True)
    picked = returned.reshape(EXPERTS * CAP, part_width)[slot_index].astype(jnp.float32)
    picked = picked.reshape(head_rows, top_count, part_width)
    moe_out = jnp.sum(picked * route_weights[:, :, None], axis=1)
    own_columns = lax.dynamic_slice_in_dim(stream_f, tp_index * part_width, part_width, 1)
    return (own_columns + moe_out).astype(jnp.bfloat16)


MESH = pl.DeviceIdType.MESH
f32 = jnp.float32
bf16 = jnp.bfloat16
SLOT_PAD = 48


def mm(a, b, dims=((1,), (0,))):
    return lax.dot_general(a.astype(bf16), b.astype(bf16), (dims, ((), ())), preferred_element_type=f32)


def mm_exact(a, b, dims=((1,), (0,))):
    return lax.dot_general(
        a.astype(f32), b.astype(f32), (dims, ((), ())), precision=highest_precision, preferred_element_type=f32
    )


def remote(src, dst, send, recv, device):
    return pltpu.make_async_remote_copy(
        src_ref=src, dst_ref=dst, send_sem=send, recv_sem=recv, device_id=device, device_id_type=MESH
    )


def greet(devices):
    barrier = pltpu.get_barrier_semaphore()
    for device in devices:
        pl.semaphore_signal(barrier, inc=1, device_id=device, device_id_type=MESH)
    pl.semaphore_wait(barrier, len(devices))


def front_kernel(
    n_sp,
    n_tp,
    ids_ref,
    query_in,
    value_in,
    ff_in,
    fb_in,
    jumps_in,
    gap_in,
    og_in,
    hg_in,
    ow_in,
    res_in,
    ng_in,
    xs_ref,
    stream_ref,
    dslot_ref,
    query_ref,
    value_ref,
    ff_ref,
    fb_ref,
    jumps_ref,
    gap_ref,
    og_ref,
    hg_ref,
    ow_ref,
    res_ref,
    ng_ref,
    in_sem,
    st,
    dec,
    rst,
    rdec,
    pos,
    rpos,
    gated,
    oacc,
    qcarry,
    pb,
    rpb,
    sq,
    rsq,
    rows,
    st_send,
    st_recv,
    dec_send,
    dec_recv,
    pos_send,
    pos_recv,
    rs_send,
    rs_recv,
    sq_send,
    sq_recv,
    ag_send,
    ag_recv,
):
    p = lax.axis_index("sp")
    t = lax.axis_index("tp")
    staged = [
        pltpu.make_async_copy(source, target, in_sem.at[i])
        for i, (source, target) in enumerate(
            (
                (ff_in, ff_ref),
                (fb_in, fb_ref),
                (gap_in, gap_ref),
                (jumps_in, jumps_ref),
                (query_in, query_ref),
                (value_in, value_ref),
                (og_in, og_ref),
                (hg_in, hg_ref),
                (res_in, res_ref),
                (ng_in, ng_ref),
                (ow_in, ow_ref),
            )
        )
    ]
    for copy in staged:
        copy.start()
    n, width = query_ref.shape
    heads = jumps_ref.shape[0]
    hw = width // heads
    n_exp = EXPERTS // n_sp
    n_z = n_sp // 2
    group = xs_ref.shape[1] // (2 * CAP)
    partner = p + 1 - 2 * lax.rem(p, 2)
    zpeers = [lax.rem(p + 2 * k, n_sp) for k in range(1, n_z)]
    zfrom = [lax.rem(p + n_sp - 2 * k, n_sp) for k in range(1, n_z)]
    speers = [lax.rem(p + k, n_sp) for k in range(1, n_sp)]
    tpeers = [lax.rem(t + k, n_tp) for k in range(1, n_tp)]
    tfrom = [lax.rem(t + n_tp - k, n_tp) for k in range(1, n_tp)]
    greet([(s, t) for s in speers] + [(p, u) for u in tpeers])

    row_i = lax.broadcasted_iota(jnp.int32, (n, n), 0)
    col_i = lax.broadcasted_iota(jnp.int32, (n, n), 1)
    lower = (col_i <= row_i).astype(f32)
    upper = (col_i >= row_i).astype(f32)
    eye = (col_i == row_i).astype(f32)

    ex_i = lax.broadcasted_iota(jnp.int32, (n, EXPERTS), 1)
    picks = [(ids_ref[:, j : j + 1] == ex_i).astype(f32) for j in range(ids_ref.shape[1])]
    named = sum(picks)
    strict_before = (row_i < col_i).astype(f32)
    named_t = mm(named, eye, ((0,), (0,)))
    rank_t = mm(named, strict_before, ((0,), (0,)))
    place = lax.rem(p, group).astype(f32) * CAP
    table = jnp.where(named_t > 0.5, rank_t + place, -1.0)
    pos[...] = jnp.full(pos.shape, -1.0, f32)
    for d in range(n_sp):
        pos[d, 0:n_exp, :] = table[d * n_exp : (d + 1) * n_exp, :]
    rank = mm(col_i < row_i, named)
    base = ex_i.astype(f32) * SLOT_PAD + rank
    lane = lax.broadcasted_iota(jnp.int32, dslot_ref.shape, 1)
    slots = jnp.zeros(dslot_ref.shape, f32)
    for j, pick in enumerate(picks):
        slots = jnp.where(lane == j, jnp.sum(pick * base, axis=1, keepdims=True), slots)
    dslot_ref[...] = slots

    for copy in staged[:6]:
        copy.wait()

    def gates(ref, index):
        key = gap_ref[index : index + 1, :] * jax.nn.sigmoid(-ref[...].astype(f32))
        return key, jnp.log1p(-key)

    key_f, log_f = gates(ff_ref, 0)
    key_b, log_b = gates(fb_ref, 1)
    sum_f = mm_exact(lower, log_f)
    sum_b = mm_exact(upper, log_b)
    jcol_f = mm_exact(lower, jumps_ref[...], ((1,), (1,)))
    jcol_b = mm_exact(upper, jumps_ref[...], ((1,), (1,)))
    jrow_f = mm_exact(jumps_ref[...], lower, ((1,), (1,)))
    jrow_b = mm_exact(jumps_ref[...], upper, ((1,), (1,)))
    query = query_ref[...].astype(f32)
    query = query * jax.nn.sigmoid(query)
    end_f, end_b = sum_f[n - 1 : n, :], sum_b[0:1, :]
    for h in range(heads):
        cols = slice(h * hw, (h + 1) * hw)
        for d, (key, total, end, jcol, jend) in enumerate(
            (
                (key_f, sum_f, end_f, jcol_f, n - 1),
                (key_b, sum_b, end_b, jcol_b, 0),
            )
        ):
            jtot = jcol[jend : jend + 1, h : h + 1]
            decay = jnp.exp(jnp.minimum(end[:, cols] - total[:, cols] + (jtot - jcol[:, h : h + 1]), 0.0))
            st[d, h * hw : (h + 1) * hw, :] = mm(
                value_ref[:, cols], key[:, cols] * decay, ((0,), (0,))
            ).astype(bf16)
            dec[d, :, cols] = jnp.broadcast_to(jnp.exp(end[:, cols] + jtot), (dec.shape[1], hw))
            qcarry[d, :, cols] = (
                query[:, cols] * jnp.exp(total[:, cols] + jcol[:, h : h + 1])
            ).astype(bf16)

    pending = []

    def go(copy):
        copy.start()
        pending.append(copy)

    st_next = 0
    for peer in [partner] + zpeers:
        way = jnp.where(peer > p, 0, 1)
        go(remote(st.at[way], rst.at[p], st_send.at[st_next], st_recv.at[p], (peer, t)))
        go(remote(dec.at[way], rdec.at[p], dec_send.at[st_next], dec_recv.at[p], (peer, t)))
        st_next += 1
    for i, peer in enumerate(speers):
        go(remote(pos.at[peer], rpos.at[p], pos_send.at[i], pos_recv.at[p], (peer, t)))

    mid_f, mid_b = sum_f[n // 2 : n // 2 + 1, :], sum_b[n // 2 : n // 2 + 1, :]
    q_f, k_f = query * jnp.exp(sum_f - mid_f), key_f * jnp.exp(mid_f - sum_f)
    q_b, k_b = query * jnp.exp(sum_b - mid_b), key_b * jnp.exp(mid_b - sum_b)
    for h in range(heads):
        cols = slice(h * hw, (h + 1) * hw)
        jump_f = jnp.exp(jnp.minimum(jcol_f[:, h : h + 1] - jrow_f[h : h + 1, :], 0.0))
        jump_b = jnp.exp(jnp.minimum(jcol_b[:, h : h + 1] - jrow_b[h : h + 1, :], 0.0))
        score = mm(q_f[:, cols], k_f[:, cols], ((1,), (1,))) * (jump_f * lower)
        score += mm(q_b[:, cols], k_b[:, cols], ((1,), (1,))) * (jump_b * upper)
        oacc[:, cols] = mm(score, value_ref[:, cols])

    def st_wait(source):
        remote(st.at[0], rst.at[source], st_send.at[0], st_recv.at[source], (partner, t)).wait_recv()
        remote(dec.at[0], rdec.at[source], dec_send.at[0], dec_recv.at[source], (partner, t)).wait_recv()

    for source in zfrom:
        st_wait(source)
        go(remote(rst.at[source], rst.at[source], st_send.at[st_next], st_recv.at[source], (partner, t)))
        go(remote(rdec.at[source], rdec.at[source], dec_send.at[st_next], dec_recv.at[source], (partner, t)))
        st_next += 1
    st_wait(partner)
    for source in zfrom:
        st_wait(source + 1 - 2 * lax.rem(p, 2))

    def carry_from(first, step, count, d):
        def one(hop, states):
            source = first + step * hop
            return tuple(
                rdec[source, 0:1, h * hw : (h + 1) * hw] * states[h]
                + rst[source, h * hw : (h + 1) * hw, :].astype(f32)
                for h in range(heads)
            )

        states = lax.fori_loop(0, count, one, tuple(jnp.zeros((hw, hw), f32) for h in range(heads)))
        for h in range(heads):
            cols = slice(h * hw, (h + 1) * hw)
            oacc[:, cols] += mm(qcarry[d, :, cols], states[h], ((1,), (1,)))

    for copy in staged[6:]:
        copy.wait()
    carry_from(0, 1, p, 0)
    carry_from(n_sp - 1, -1, n_sp - 1 - p, 1)

    for h in range(heads):
        cols = slice(h * hw, (h + 1) * hw)
        out = oacc[:, cols]
        scale = lax.rsqrt(jnp.mean(out * out, axis=-1, keepdims=True) + eps_norm)
        gate = og_ref[:, cols].astype(f32)
        gated[:, cols] = (out * scale * hg_ref[:, cols] * (gate * jax.nn.sigmoid(gate))).astype(bf16)

    for u in range(n_tp):
        pb[u] = mm(gated[...], ow_ref[:, u * width : (u + 1) * width]).astype(bf16)
    for i, peer in enumerate(tpeers):
        go(remote(pb.at[peer], rpb.at[t], rs_send.at[i], rs_recv.at[t], (p, peer)))
    own = pl.ds(pl.multiple_of(t * width, 128), width)
    total = pb[t].astype(f32)
    for source in tfrom:
        remote(pb.at[0], rpb.at[source], rs_send.at[0], rs_recv.at[source], (p, tpeers[0])).wait_recv()
        total = total + rpb[source].astype(f32)
    stream = (res_ref[:, own].astype(f32) + total).astype(bf16)
    stream_ref[...] = stream
    stream = stream.astype(f32)
    sq[...] = mm_exact(jnp.ones((sq.shape[0], width), f32), stream * stream, ((1,), (1,)))
    for i, peer in enumerate(tpeers):
        go(remote(sq, rsq.at[t], sq_send.at[i], sq_recv.at[t], (p, peer)))
    squares = sq[...]
    for source in tfrom:
        remote(sq, rsq.at[source], sq_send.at[0], sq_recv.at[source], (p, tpeers[0])).wait_recv()
        squares = squares + rsq[source]
    scale = lax.rsqrt(squares / (width * n_tp) + eps_norm)
    scale = mm_exact(eye, scale, ((1,), (1,)))[:, 0:1]
    rows[p, t] = (stream * scale * ng_ref[:, own]).astype(bf16)

    ag_next = 0
    xn = t + 1 - 2 * lax.rem(t, 2)
    yn = lax.rem(t + 2, n_tp)
    dg = n_tp - 1 - t
    cut = n // 2

    def view(block, share, part):
        ref = rows.at[block, share]
        return ref if part is None else ref.at[pl.ds(part * cut, cut)]

    def spread(block, share, part, device):
        nonlocal ag_next
        ref = view(block, share, part)
        go(remote(ref, ref, ag_send.at[ag_next], ag_recv.at[block, share, part or 0], device))
        ag_next += 1

    def arrive(block, share, part=None):
        ref = view(block, share, part)
        remote(ref, ref, ag_send.at[0], ag_recv.at[block, share, part or 0], (partner, t)).wait_recv()

    def across(block):
        spread(block, t, 0, (p, xn))
        spread(block, t, 1, (p, yn))
        spread(block, t, 1, (p, xn))
        spread(block, t, 0, (p, yn))
        spread(block, t, None, (partner, t))

    def relay(block):
        arrive(block, xn, 0)
        spread(block, xn, 0, (p, yn))
        arrive(block, yn, 1)
        spread(block, yn, 1, (p, xn))

    for peer in zpeers:
        spread(p, t, None, (peer, t))
    across(p)
    for block in zfrom:
        arrive(block, t)
        across(block)
    for block in [p] + zfrom:
        relay(block)
    for block in [p] + zfrom:
        arrive(block, xn, 1)
        spread(block, xn, None, (partner, t))
        arrive(block, yn, 0)
        spread(block, yn, None, (partner, t))
        arrive(block, dg, 0)
        arrive(block, dg, 1)
        spread(block, dg, None, (partner, t))
    for source in speers:
        remote(pos.at[0], rpos.at[source], pos_send.at[0], pos_recv.at[source], (partner, t)).wait_recv()
    rpos[p] = pos[p]
    for block in [p] + zfrom:
        other = block + 1 - 2 * lax.rem(p, 2)
        arrive(other, t)
        for share in (xn, yn, dg):
            arrive(other, share)

    half = group * CAP
    slot_i = lax.broadcasted_iota(jnp.int32, (half, n), 0).astype(f32)
    for e in range(n_exp):
        for g in range(n_sp // group):
            hot = [(slot_i == rpos[g * group + b, e : e + 1, :]).astype(bf16) for b in range(group)]

            def one(u, unused, hot=hot, g=g, e=e):
                part = mm(hot[0], rows[g * group, u])
                for b in range(1, group):
                    part = part + mm(hot[b], rows[g * group + b, u])
                xs_ref[
                    e, g * half : (g + 1) * half, pl.ds(pl.multiple_of(u * width, 128), width)
                ] = part.astype(bf16)
                return unused

            lax.fori_loop(0, n_tp, one, 0)
    for copy in pending:
        copy.wait_send()


def expert_kernel(
    n_sp,
    n_tp,
    xs_ref,
    wg_ref,
    wu_ref,
    wd_ref,
    stream_ref,
    dslot_ref,
    rw_ref,
    out_ref,
    gbuf,
    ubuf,
    wd,
    acts,
    prod,
    rprod,
    wsem,
    dsem,
    act_send,
    act_recv,
    ret_send,
    ret_recv,
):
    p = lax.axis_index("sp")
    t = lax.axis_index("tp")
    n_exp, depth, hidden = wg_ref.shape
    slots = xs_ref.shape[1]
    tile = gbuf.shape[2]
    tiles = hidden // tile
    xn = t + 1 - 2 * lax.rem(t, 2)
    yn = lax.rem(t + 2, n_tp)
    dg = n_tp - 1 - t
    speers = [lax.rem(p + k, n_sp) for k in range(1, n_sp)]
    half = slots // 2
    halves = (pl.ds(0, half), pl.ds(half, half))

    def fetch(step, slot):
        e, i = step // tiles, lax.rem(step, tiles)
        cols = pl.ds(pl.multiple_of(i * tile, 128), tile)
        return (
            pltpu.make_async_copy(wg_ref.at[e, :, cols], gbuf.at[slot], wsem.at[0, slot]),
            pltpu.make_async_copy(wu_ref.at[e, :, cols], ubuf.at[slot], wsem.at[1, slot]),
        )

    for step in range(2):
        for copy in fetch(step, step):
            copy.start()
    down = [pltpu.make_async_copy(wd_ref.at[e], wd.at[e], dsem.at[e]) for e in range(n_exp)]
    greet([(s, t) for s in speers] + [(p, xn), (p, yn)])
    prod[...] = jnp.zeros(prod.shape, bf16)

    def act_copy(e, block, part, number, device):
        ref = acts.at[e, block, halves[part]]
        return remote(ref, ref, act_send.at[e, number], act_recv.at[e, block, part], (p, device))

    def own_sends(e):
        return (
            act_copy(e, t, 0, 0, xn),
            act_copy(e, t, 1, 1, yn),
            act_copy(e, t, 1, 2, xn),
            act_copy(e, t, 0, 3, yn),
        )

    def expert(e, unused):
        def part(i, unused):
            step = e * tiles + i
            slot = lax.rem(step, 2)
            for copy in fetch(step, slot):
                copy.wait()
            x = xs_ref[e]
            gate = jnp.dot(x, gbuf[slot], preferred_element_type=f32)
            up = jnp.dot(x, ubuf[slot], preferred_element_type=f32)
            gate = jnp.minimum(gate, limit_value)
            up = jnp.clip(up, -limit_value, limit_value)
            cols = pl.ds(pl.multiple_of(i * tile, 128), tile)
            acts[e, t, :, cols] = (gate * jax.nn.sigmoid(alpha_value * gate) * (up + 1.0)).astype(bf16)

            @pl.when(step + 2 < n_exp * tiles)
            def _():
                for copy in fetch(step + 2, slot):
                    copy.start()

            return unused

        lax.fori_loop(0, tiles, part, 0)
        for copy in own_sends(e):
            copy.start()
        return unused

    lax.fori_loop(0, n_exp, expert, 0)
    for copy in down:
        copy.start()

    def forward(e, unused):
        act_copy(e, xn, 0, 0, xn).wait_recv()
        act_copy(e, xn, 0, 4, yn).start()
        act_copy(e, yn, 1, 0, xn).wait_recv()
        act_copy(e, yn, 1, 5, xn).start()
        return unused

    lax.fori_loop(0, n_exp, forward, 0)
    for copy in down:
        copy.wait()

    def ret_copy(e, i, peer):
        return remote(prod.at[e, peer], rprod.at[p, e], ret_send.at[e, i], ret_recv.at[e, p], (peer, t))

    def lower(e, unused):
        act_copy(e, xn, 1, 0, xn).wait_recv()
        act_copy(e, yn, 0, 0, xn).wait_recv()
        act_copy(e, dg, 0, 0, xn).wait_recv()
        act_copy(e, dg, 1, 0, xn).wait_recv()
        total = jnp.dot(acts[e, 0], wd[e, 0:hidden, :], preferred_element_type=f32)
        for u in range(1, n_tp):
            total += jnp.dot(acts[e, u], wd[e, u * hidden : (u + 1) * hidden, :], preferred_element_type=f32)
        for s in range(n_sp):
            prod[e, s, 0:CAP, :] = total[s * CAP : (s + 1) * CAP, :].astype(bf16)
        for i, peer in enumerate(speers):
            ret_copy(e, i, peer).start()
        rprod[p, e] = prod[e, p]
        return unused

    lax.fori_loop(0, n_exp, lower, 0)

    tokens, width = stream_ref.shape
    total = stream_ref[...].astype(f32)
    lane = lax.broadcasted_iota(jnp.int32, (tokens, n_exp * SLOT_PAD), 1).astype(f32)

    def returns(k, total):
        source = lax.rem(p + n_sp - k, n_sp)

        @pl.when(k > 0)
        def _():
            for e in range(n_exp):
                remote(
                    prod.at[e, 0], rprod.at[source, e], ret_send.at[e, 0], ret_recv.at[e, source], (speers[0], t)
                ).wait_recv()

        first = (source * (n_exp * SLOT_PAD)).astype(f32)
        mix = jnp.zeros(lane.shape, f32)
        for j in range(rw_ref.shape[1]):
            mix += jnp.where(dslot_ref[:, j : j + 1] - first == lane, rw_ref[:, j : j + 1], 0.0)
        high = mix.astype(bf16)
        low = (mix - high.astype(f32)).astype(bf16)
        block = rprod[source].reshape(n_exp * SLOT_PAD, width)
        return (
            total
            + jnp.dot(high, block, preferred_element_type=f32)
            + jnp.dot(low, block, preferred_element_type=f32)
        )

    total = lax.fori_loop(0, n_sp, returns, total)
    out_ref[...] = total.astype(bf16)

    def drain(e, unused):
        for copy in own_sends(e):
            copy.wait_send()
        act_copy(e, xn, 0, 4, yn).wait_send()
        act_copy(e, yn, 1, 5, xn).wait_send()
        for i, peer in enumerate(speers):
            ret_copy(e, i, peer).wait_send()
        return unused

    lax.fori_loop(0, n_exp, drain, 0)


def fused(
    n_sp,
    n_tp,
    residual,
    query_in,
    value_in,
    forget_fwd,
    forget_bwd,
    jumps,
    gate_gap,
    out_gate,
    head_gain,
    out_weight,
    norm_gain,
    route_ids,
    route_weights,
    w_gate,
    w_up,
    w_down,
):
    tokens, width = query_in.shape
    heads = jumps.shape[0]
    hw = width // heads
    n_exp, model, hidden = w_gate.shape
    slots = n_sp * CAP
    vmem = pl.BlockSpec(memory_space=pltpu.VMEM)
    dma = pltpu.SemaphoreType.DMA
    group = n_sp // 2
    n_ag = (n_sp // 2) * n_tp * 3
    xs, stream, dslot = pl.pallas_call(
        functools.partial(front_kernel, n_sp, n_tp),
        out_shape=(
            jax.ShapeDtypeStruct((n_exp, slots, model), bf16),
            jax.ShapeDtypeStruct((tokens, width), bf16),
            jax.ShapeDtypeStruct((tokens, 128), f32),
        ),
        in_specs=[vmem] + [pl.BlockSpec(memory_space=pl.ANY)] * 11,
        out_specs=(vmem, vmem, vmem),
        scratch_shapes=[
            pltpu.VMEM((tokens, width), bf16),
            pltpu.VMEM((tokens, width), bf16),
            pltpu.VMEM((tokens, width), bf16),
            pltpu.VMEM((tokens, width), bf16),
            pltpu.VMEM(jumps.shape, f32),
            pltpu.VMEM(gate_gap.shape, f32),
            pltpu.VMEM((tokens, width), bf16),
            pltpu.VMEM((1, width), f32),
            pltpu.VMEM(out_weight.shape, bf16),
            pltpu.VMEM((tokens, model), bf16),
            pltpu.VMEM((1, model), f32),
            dma((11,)),
            pltpu.VMEM((2, heads * hw, hw), bf16),
            pltpu.VMEM((2, 8, width), f32),
            pltpu.VMEM((n_sp, heads * hw, hw), bf16),
            pltpu.VMEM((n_sp, 8, width), f32),
            pltpu.VMEM((n_sp, 8, tokens), f32),
            pltpu.VMEM((n_sp, 8, tokens), f32),
            pltpu.VMEM((tokens, width), bf16),
            pltpu.VMEM((tokens, width), f32),
            pltpu.VMEM((2, tokens, width), bf16),
            pltpu.VMEM((n_tp, tokens, width), bf16),
            pltpu.VMEM((n_tp, tokens, width), bf16),
            pltpu.VMEM((8, tokens), f32),
            pltpu.VMEM((n_tp, 8, tokens), f32),
            pltpu.VMEM((n_sp, n_tp, tokens, width), bf16),
            dma((n_sp,)),
            dma((n_sp,)),
            dma((n_sp,)),
            dma((n_sp,)),
            dma((n_sp,)),
            dma((n_sp,)),
            dma((n_tp,)),
            dma((n_tp,)),
            dma((n_tp,)),
            dma((n_tp,)),
            dma((n_ag,)),
            dma((n_sp, n_tp, 2)),
        ],
        compiler_params=pltpu.CompilerParams(
            collective_id=0, has_side_effects=True, vmem_limit_bytes=60 * 1024 * 1024
        ),
        name="front",
    )(
        route_ids,
        query_in,
        value_in,
        forget_fwd,
        forget_bwd,
        jumps,
        gate_gap,
        out_gate,
        head_gain.reshape(1, width),
        out_weight,
        residual,
        norm_gain.reshape(1, model),
    )
    tile = math.gcd(hidden, 512)
    anywhere = pl.BlockSpec(memory_space=pl.ANY)
    return pl.pallas_call(
        functools.partial(expert_kernel, n_sp, n_tp),
        out_shape=jax.ShapeDtypeStruct((tokens, width), bf16),
        in_specs=[vmem, anywhere, anywhere, anywhere, vmem, vmem, vmem],
        out_specs=vmem,
        scratch_shapes=[
            pltpu.VMEM((2, model, tile), bf16),
            pltpu.VMEM((2, model, tile), bf16),
            pltpu.VMEM((n_exp, hidden * n_tp, width), bf16),
            pltpu.VMEM((n_exp, n_tp, slots, hidden), bf16),
            pltpu.VMEM((n_exp, n_sp, SLOT_PAD, width), bf16),
            pltpu.VMEM((n_sp, n_exp, SLOT_PAD, width), bf16),
            dma((2, 2)),
            dma((n_exp,)),
            dma((n_exp, 6)),
            dma((n_exp, n_tp, 2)),
            dma((n_exp, n_sp)),
            dma((n_exp, n_sp)),
        ],
        compiler_params=pltpu.CompilerParams(
            collective_id=1, has_side_effects=True, vmem_limit_bytes=60 * 1024 * 1024
        ),
        name="experts",
    )(xs, w_gate, w_up, w_down, stream, dslot, route_weights)


def solution(mesh):
    n_sp, n_tp = mesh.shape["sp"], mesh.shape["tp"]
    square = n_tp == 4 and n_sp % 2 == 0 and n_sp <= 8
    program = functools.partial(fused, n_sp, n_tp) if square else shards

    return jax.shard_map(
        program,
        mesh=mesh,
        in_specs=(
            P("sp", None),
            P("sp", "tp"),
            P("sp", "tp"),
            P("sp", "tp"),
            P("sp", "tp"),
            P("tp", "sp"),
            P(None, "tp"),
            P("sp", "tp"),
            P("tp"),
            P("tp", None),
            P(),
            P("sp", None),
            P("sp", None),
            P("sp", None, "tp"),
            P("sp", None, "tp"),
            P("sp", None, "tp"),
        ),
        out_specs=P("sp", "tp"),
        check_vma=False,
    )
```
